32 devices in a mesh: sp: 8 (over z, y), tp: 4 (over x, core).
Axes of the slice: x: 2, y: 2, z: 4, core: 2. Of those that a mesh axis runs over, the one named last changes fastest.
Arguments:
- tokens: bfloat16 [1280, 2048], P('sp'), may hold values from -8 to 8
- query_weight: bfloat16 [2048, 2048], P('sp', 'tp'), may hold values from -0.5 to 0.5
- key_weight: bfloat16 [2048, 2048], P('sp', 'tp'), may hold values from -0.5 to 0.5
- value_weight: bfloat16 [2048, 2048], P('sp', 'tp'), may hold values from -0.125 to 0.125
- out_weight: bfloat16 [2048, 2048], P('tp', 'sp'), may hold values from -0.125 to 0.125
- mix_lambda: float32 [16], P('tp'), may hold values from 0.3 to 0.8
- head_gain: float32 [128], replicated, may hold values from 0.1 to 1.9
Outputs:
- attended: bfloat16 [1280, 2048], P('sp')
The draws below stay inside these ranges and needn't reach their ends.
All inputs are finite; a program needn't handle non-finite values.
Results may differ from the reference program's by a relative error of at most 0.018.
The reference program's roundings to bfloat16 on the way (of `queries`, `keys`, `values` and `head_out`) count: a program that leaves them out, or rounds other values in their place, can miss the bound.
Values may be sent and summed in bfloat16 or wider, within the bound.
A program may use at most 192 MiB of HBM per device.

```python
import math
import jax
import jax.numpy as jnp
from jax import lax

D = 2048
HEADS = 16
QKD = 64
VDIM = 128
TOK_DEV = 160
SEQ = 1280


def draw_tokens(key, part):
    noise_key, mean_key = jax.random.split(key, 2)
    block_count = SEQ // TOK_DEV
    base = jnp.clip(jax.random.normal(noise_key, (SEQ, D), jnp.float32), -4.0, 4.0)
    offsets = jnp.clip(0.7 * jax.random.normal(mean_key, (block_count, D), jnp.float32), -2.0, 2.0)
    drawn = base + jnp.repeat(offsets, TOK_DEV, axis=0)
    return drawn.astype(jnp.bfloat16)


def projection_draw(key, salt):
    spread = (D * 6 // 7) ** (-0.5)
    noise = spread * jax.random.normal(jax.random.fold_in(key, salt), (D, HEADS * 2 * QKD), jnp.float32)
    drawn = jnp.clip(noise, -0.5, 0.5)
    return drawn.astype(jnp.bfloat16)


def draw_query_weight(key, part):
    return projection_draw(key, 101)


def draw_key_weight(key, part):
    return projection_draw(key, 202)


def block_levels(own_key, shape, pieces, low, high):
    loudness = 1.0
    for axis_at, shards_of in pieces:
        steps = jax.random.uniform(jax.random.fold_in(jax.random.fold_in(own_key, 6), axis_at), (shards_of,), jnp.float32, low / len(pieces), high / len(pieces))
        loudness = loudness * jnp.repeat(jnp.exp(steps), shape[axis_at] // shards_of).reshape((-1,) + (1,) * (len(shape) - 1 - axis_at))
    return loudness


def normal_values(key, shape, scale, most, shards=(), kind=jnp.bfloat16):
    entries = jax.random.normal(key, shape, jnp.float32) * scale
    if len(shards) > 0:
        entries = block_levels(key, shape, shards, -0.22, 0.18) * entries
    return jnp.clip(entries, min=-most, max=most).astype(kind)


def setup_inputs(seed: int = 0) -> dict:
    splits = jax.random.split(jax.random.key(seed), 8)
    return {
        "tokens": draw_tokens(jax.random.fold_in(splits[7], 71), 0),
        "query_weight": draw_query_weight(jax.random.fold_in(splits[7], 71), 0),
        "key_weight": draw_key_weight(jax.random.fold_in(splits[7], 71), 0),
        "value_weight": normal_values(splits[3], (D, HEADS * VDIM), D ** -0.5, 0.125, ((0, 8), (1, 4))),
        "out_weight": normal_values(splits[4], (HEADS * VDIM, D), (HEADS * VDIM) ** -0.5, 0.125, ((0, 4), (1, 8))),
        "mix_lambda": jnp.clip(0.3 + 0.5 * jax.random.uniform(splits[5], (HEADS,), jnp.float32) ** block_levels(splits[5], (HEADS,), ((0, 4),), -0.2, 0.2), 0.3, 0.8),
        "head_gain": jnp.clip(1.0 + 0.18 * jax.random.normal(splits[6], (VDIM,), jnp.float32), 0.1, 1.9),
    }


def reference(tokens, query_weight, key_weight, value_weight, out_weight, mix_lambda, head_gain):
    length = tokens.shape[0]
    queries = jnp.dot(tokens, query_weight, preferred_element_type=jnp.float32).astype(jnp.bfloat16)
    keys = jnp.dot(tokens, key_weight, preferred_element_type=jnp.float32).astype(jnp.bfloat16)
    values = jnp.dot(tokens, value_weight, preferred_element_type=jnp.float32).astype(jnp.bfloat16)
    queries = queries.reshape(length, HEADS, 2, QKD)
    keys32 = keys.reshape(length, HEADS, 2, QKD).astype(jnp.float32)
    values32 = values.reshape(length, HEADS, VDIM).astype(jnp.float32)
    block_size = math.gcd(length, 512)
    block_count = length // block_size
    score_scale = QKD ** (-0.5)
    key_pos = jnp.arange(length, dtype=jnp.int32)

    def one_block(block_index):
        first_row = (block_index * block_size).astype(jnp.int32)
        query_rows = lax.dynamic_slice_in_dim(queries, first_row, block_size, 0).astype(jnp.float32)
        scores = jnp.einsum('qhcd,khcd->hcqk', query_rows, keys32) * score_scale
        query_pos = first_row + jnp.arange(block_size, dtype=jnp.int32)
        visible = key_pos[None, :] <= query_pos[:, None]
        scores = jnp.where(visible, scores, -jnp.inf)
        probabilities = jax.nn.softmax(scores, axis=-1)
        weights = probabilities[:, 0] - mix_lambda[:, None, None] * probabilities[:, 1]
        mixture = jnp.einsum('hqk,khd->qhd', weights, values32)
        normalized = mixture * lax.rsqrt(lax.optimization_barrier(jnp.mean(mixture * mixture, axis=-1, keepdims=True)) + 1e-05) * head_gain
        return normalized.astype(jnp.bfloat16)
    head_out = lax.map(one_block, jnp.arange(block_count, dtype=jnp.int32))
    head_out = head_out.reshape(length, HEADS * VDIM)
    return jnp.dot(head_out, out_weight, preferred_element_type=jnp.float32).astype(jnp.bfloat16)
```

```python
import functools

import jax
import jax.numpy as jnp
from jax import lax
from jax.experimental import pallas as pl
from jax.experimental.pallas import tpu as pltpu
from jax.sharding import PartitionSpec as P

MESH = pl.DeviceIdType.MESH
Q, K, V = 0, 1, 2
PLAN = (
    "yk", "t0", "Wk1", "Wk3", "Wv3", "t1", "Wv1", "Wk2", "Wv2", "fk1", "yv", "Wq2", "t2", "m2",
    "Wq1", "fv1", "fk3", "fk2", "m1", "yq", "Wq3", "t3", "e2", "O", "fv2", "fv3", "m3", "fq2", "e3",
    "e1", "fq1", "gv", "hv", "fq3", "dv", "gk", "gq", "hq", "hk", "dk", "o1", "dq", "a0", "a1",
    "a3", "a2", "r0", "o2", "r1", "r2", "r3", "H", "P10", "S10", "o3", "P11", "P01", "S11", "P00",
    "S01", "X10", "S00", "X11", "F0", "X01", "F1", "X00", "Z",
)


def kernel(
    n, parts, heads,
    tok, wq, wk, wv, wo_in, lam, gain, out,
    x, w, acc, qb, kb, vb, wo, ho_out, ho, part_out, part_in, sum_out, sum_in, staged,
    local_sem, xs_send, xs_recv, xt_send, w_send, wf_send, w_recv,
    kv_send, kv_recv, wo_send, wo_recv, ho_send, ho_recv,
    hof_send, hof_recv, p_send, p_recv, s_send, s_recv, f_send, f_recv, d_send, d_recv,
):
    groups = n // heads
    s, t = lax.axis_index("sp"), lax.axis_index("tp")
    h, r = lax.div(s, groups), lax.rem(s, groups)
    rows, width = tok.shape
    depth = wq.shape[0]
    vdim = gain.shape[-1]
    seg = width // parts
    ocols = wo_in.shape[1]
    bits = [1 << i for i in range(parts.bit_length() - 1)]
    chunks = xs_recv.shape[2]
    by_source = depth % 128 == 0

    def at_sp(index):
        return (index, t)

    def at_tp(index):
        return (s, index)

    def flip(index, bit):
        return index + bit - 2 * bit * lax.rem(lax.div(index, bit), 2)

    def ds(index, size):
        return pl.ds(pl.multiple_of(index * size, size), size)

    pending = []

    def send(src, dst, send_sem, recv_sem, device, cond=None):
        copy = pltpu.make_async_remote_copy(
            src_ref=src, dst_ref=dst, send_sem=send_sem, recv_sem=recv_sem,
            device_id=device, device_id_type=MESH,
        )
        if cond is None:
            copy.start()
        else:
            pl.when(cond)(copy.start)
        pending.append((copy, cond))

    def arrived(ref, sem):
        pltpu.make_async_copy(ref, ref, sem).wait()

    barrier = pltpu.get_barrier_semaphore()
    for d in range(1, heads):
        pl.semaphore_signal(
            barrier, inc=1, device_id=at_sp(lax.rem(h + d, heads) * groups + r), device_id_type=MESH
        )
    for d in range(1, groups):
        pl.semaphore_signal(
            barrier, inc=1, device_id=at_sp(h * groups + lax.rem(r + d, groups)), device_id_type=MESH
        )
    for bit in bits:
        pl.semaphore_signal(barrier, inc=1, device_id=at_tp(flip(t, bit)), device_id_type=MESH)
    pl.semaphore_wait(barrier, heads + groups - 2 + len(bits))

    def x_at(block, part, c):
        return x.at[ds(block * chunks + c, rows // chunks), ds(part, seg)]

    def w_at(block, i):
        return w.at[i, ds(block, depth), :]

    right, left = at_sp(s + groups), at_sp(s - groups)
    can_right, can_left = h + 1 < heads, h > 0
    weights = (wq, wk, wv)
    peers = [at_sp(h * groups + lax.rem(r + e, groups)) for e in range(1, groups)]
    others = [lax.rem(r + e, groups) for e in range(1, groups)]

    def send_weight(i, d):
        ref = weights[i]
        for owner, cond in ((h + d, h + d < heads), (h - d, h - d >= 0)):
            safe = jnp.where(cond, owner, h)
            send(
                ref.at[:, ds(safe, vdim)], w_at(s, i),
                w_send.at[safe, i], w_recv.at[s, i], at_sp(safe * groups + r), cond,
            )

    chunk = rows // chunks
    onward = ((right, can_right), (left, can_left))

    def send_tokens():
        for c in range(chunks):
            for side, (target, can) in enumerate(onward):
                send(tok.at[pl.ds(c * chunk, chunk), ds(t, seg)], x_at(h, t, c),
                     xs_send.at[0, side, c], xs_recv.at[h, t, c], target, can)

    def send_own_weight(i):
        for e, peer in enumerate(peers):
            send(
                weights[i].at[:, ds(h, vdim)], w_at(s, i),
                wf_send.at[h, e, i], w_recv.at[s, i], peer,
            )

    locals_ = [
        pltpu.make_async_copy(ref.at[:, ds(h, vdim)], w_at(s, i), local_sem.at[i])
        for i, ref in enumerate(weights)
    ]
    locals_.append(pltpu.make_async_copy(tok, x.at[ds(h, rows), :], local_sem.at[3]))
    locals_.append(pltpu.make_async_copy(wo_in, wo.at[h], local_sem.at[4]))
    for copy in locals_:
        copy.start()

    def reach(k):
        return [
            (jnp.where(have, block, h), have, side)
            for side, (block, have) in enumerate(((h - k, h - k >= 0), (h + k, h + k < heads)))
        ]

    spread = [(v, [b for b in reversed(bits) if v == 0 or b < (v & -v)]) for v in range(parts)]
    spread.sort(key=lambda item: -(item[0] & -item[0]) if item[0] else -parts)
    slot_of = {}
    for v, along in spread:
        for b in along:
            slot_of[v, b] = len(slot_of)

    def part_of(v):
        part = t
        for b in bits:
            if v & b:
                part = flip(part, b)
        return part

    def pass_on(block, v, along, c, cond):
        piece = x_at(block, part_of(v), c)
        for b in along:
            send(piece, piece, xt_send.at[block, slot_of[v, b], c], xs_recv.at[block, part_of(v), c],
                 at_tp(flip(t, b)), cond)

    def token_wait(block, v, c, cond):
        def body():
            arrived(x_at(block, part_of(v), c), xs_recv.at[block, part_of(v), c])

        pl.when(cond)(body)

    def relay_tokens(k):
        for c in range(chunks):
            for safe, have, side in reach(k):
                token_wait(safe, 0, c, have)
                if k < heads - 1:
                    target, can = onward[side]
                    send(x_at(safe, t, c), x_at(safe, t, c), xs_send.at[k, side, c],
                         xs_recv.at[safe, t, c], target, jnp.logical_and(have, can))
                pass_on(safe, 0, spread[0][1], c, have)

    def spread_tokens(k, last):
        for v, along in spread[1:]:
            if bool(along) == last:
                continue
            for c in range(chunks):
                for safe, have, _ in reach(k):
                    token_wait(safe, v, c, have)
                    pass_on(safe, v, along, c, have)

    def forward_weight(i, d):
        for source_h, have, _ in reach(d):
            source = source_h * groups + r

            def wait_piece(source=source):
                arrived(w_at(source, i), w_recv.at[source, i])

            pl.when(have)(wait_piece)
            for e, peer in enumerate(peers):
                send(w_at(source, i), w_at(source, i), wf_send.at[source_h, e, i],
                     w_recv.at[source, i], peer, have)

    def have_weight(i):
        for other in others:
            for k in range(heads):
                source = k * groups + other
                arrived(w_at(source, i), w_recv.at[source, i])

    def product(i, group):
        total = None
        for k in range(heads):
            source = k * groups + group
            term = jnp.dot(
                x[:, ds(source, depth)], w[i, ds(source, depth), :], preferred_element_type=jnp.float32
            )
            total = term if total is None else total + term
        return total

    def finish(i):
        if not by_source:
            return jnp.dot(x[...], w[i], preferred_element_type=jnp.float32).astype(jnp.bfloat16)
        if groups > 2:
            def body(e, carry):
                acc[i] += product(i, lax.rem(r + e, groups))
                return carry

            lax.fori_loop(1, groups - 1, body, 0)
        return (acc[i] + product(i, lax.rem(r + groups - 1, groups))).astype(jnp.bfloat16)

    def share_rows(i, buf):
        full = finish(i)
        for k in range(heads):
            block = k * groups + r
            here = buf.at[ds(block, rows), :]
            buf[ds(block, rows), :] = full[k * rows:(k + 1) * rows, :]
            for e, peer in enumerate(peers):
                send(here, here, kv_send.at[i - 1, k, e], kv_recv.at[i - 1, block], peer)

    def send_out_weight():
        send(wo_in, wo.at[h], wo_send.at[0, 0], wo_recv.at[h], right, can_right)
        send(wo_in, wo.at[h], wo_send.at[0, 1], wo_recv.at[h], left, can_left)

    def relay_out_weight(k):
        for safe, have, side in reach(k):

            def wait_piece(safe=safe):
                arrived(wo.at[safe], wo_recv.at[safe])

            pl.when(have)(wait_piece)
            if k < heads - 1:
                target, can = onward[side]
                send(wo.at[safe], wo.at[safe], wo_send.at[k, side], wo_recv.at[safe], target,
                     jnp.logical_and(have, can))

    lane = lax.broadcasted_iota(jnp.int32, (rows, vdim), 1)
    factor = (vdim // 2) ** (-0.5) * 1.4426950408889634
    lam_here = jnp.float32(0.0)
    for k in range(heads):
        lam_here = jnp.where(h == k, lam[k], lam_here)
    seen = []

    def attend(k):
        for j in range(k + 1):
            if j in seen:
                continue
            seen.append(j)
            for other in others:
                block = j * groups + other
                arrived(kb.at[ds(block, rows), :], kv_recv.at[0, block])
                arrived(vb.at[ds(block, rows), :], kv_recv.at[1, block])
        extent = (k + 1) * groups * rows
        q_rows = qb[k * rows:(k + 1) * rows, :]
        keys = kb[:extent, :]
        values = vb[:extent, :]
        ahead = lax.broadcasted_iota(jnp.int32, (rows, extent), 1) - lax.broadcasted_iota(
            jnp.int32, (rows, extent), 0
        )
        visible = ahead <= (k * groups + r) * rows
        maps = []
        for c in range(2):
            picked = jnp.where((lane >= vdim // 2) == (c == 1), q_rows, jnp.zeros_like(q_rows))
            scores = lax.dot_general(
                picked, keys, (((1,), (1,)), ((), ())), preferred_element_type=jnp.float32
            )
            scores = jnp.where(visible, scores, -1e30)
            top = jnp.max(scores, axis=-1, keepdims=True)
            e = jnp.exp2((scores - top) * factor)
            total = jnp.sum(e, axis=-1, keepdims=True)
            mixed = jnp.dot(e.astype(jnp.bfloat16), values, preferred_element_type=jnp.float32)
            maps.append(mixed / total)
        mixture = maps[0] - lam_here * maps[1]
        normalized = (
            mixture
            * lax.rsqrt(jnp.mean(mixture * mixture, axis=-1, keepdims=True) + 1e-05)
            * gain[...]
        )
        ho_out[k] = normalized.astype(jnp.bfloat16)
        send(ho_out.at[k], ho.at[r, h], ho_send.at[k], ho_recv.at[h], at_sp(k * groups + r), k != h)

        @pl.when(k == h)
        def _():
            ho[r, h] = ho_out[k]

    def begin(i):
        for copy in locals_:
            copy.wait()
        locals_.clear()
        if by_source:
            acc[i] = product(i, r)

    def queries():
        qb[...] = finish(Q)

    def forward_heads(d):
        for source, have, _ in reach(d) if d else [(h, None, 0)]:
            if d:

                def wait_piece(source=source):
                    arrived(ho.at[r, source], ho_recv.at[source])

                pl.when(have)(wait_piece)
            for e, peer in enumerate(peers):
                send(ho.at[r, source], ho.at[r, source], hof_send.at[e, source],
                     hof_recv.at[r, source], peer, have)

    def have_heads():
        for other in others:
            for k in range(heads):
                arrived(ho.at[other, k], hof_recv.at[other, k])

    low = lax.rem(t, 2)
    buddy = at_tp(flip(t, 1))
    pairs = heads // 2
    members = [r] + others

    def column_block(p, which):
        return 2 * lax.rem(lax.div(h, 2) + p, pairs) + lax.rem(h + which, 2)

    def which_rows(later):
        return range(1, groups) if later else range(1)

    def partial_product(e, p, which):
        lhs = jnp.concatenate([ho[members[e], k] for k in range(heads)], axis=-1)
        return jnp.dot(lhs, wo[column_block(p, which)], preferred_element_type=jnp.float32)

    def project_theirs(later, p):
        for e in which_rows(later):
            j = e * pairs + p
            part_out[j] = partial_product(e, p, 1 - low).astype(jnp.bfloat16)
            send(part_out.at[j], part_in.at[j], p_send.at[j], p_recv.at[j], buddy)

    def project_mine(later, p):
        for e in which_rows(later):
            j = e * pairs + p
            own = partial_product(e, p, low)
            arrived(part_in.at[j], p_recv.at[j])
            sum_out[0, j] = (own + part_in[j].astype(jnp.float32)).astype(jnp.bfloat16)
            send(sum_out.at[0, j], sum_in.at[0, j], s_send.at[0, j], s_recv.at[0, j],
                 at_tp(flip(t, bits[1])))

    def add_up(later, p):
        for e in which_rows(later):
            j = e * pairs + p
            for i in range(1, len(bits)):
                arrived(sum_in.at[i - 1, j], s_recv.at[i - 1, j])
                total = (
                    sum_out[i - 1, j].astype(jnp.float32) + sum_in[i - 1, j].astype(jnp.float32)
                ).astype(jnp.bfloat16)
                if i + 1 < len(bits):
                    sum_out[i, j] = total
                    send(sum_out.at[i, j], sum_in.at[i, j], s_send.at[i, j], s_recv.at[i, j],
                         at_tp(flip(t, bits[i + 1])))
            column = column_block(p, low) * groups + r
            if e == 0:
                staged[column] = total
                send(staged.at[column], staged.at[column], d_send.at[column], d_recv.at[column], buddy)
            else:
                sum_out[len(bits) - 1, j] = total
                send(sum_out.at[len(bits) - 1, j], staged.at[column], f_send.at[j], f_recv.at[column],
                     peers[e - 1])

    def finished(p):
        for other in others:
            column = column_block(p, low) * groups + other
            arrived(staged.at[column], f_recv.at[column])
            send(staged.at[column], staged.at[column], d_send.at[column], d_recv.at[column], buddy)

    def all_finished():
        for group in members:
            for p in range(pairs):
                column = column_block(p, 1 - low) * groups + group
                arrived(staged.at[column], d_recv.at[column])

    index = {"q": Q, "k": K, "v": V}
    run = {
        "t": lambda k: relay_tokens(int(k)) if int(k) else send_tokens(),
        "m": lambda k: spread_tokens(int(k), False),
        "e": lambda k: spread_tokens(int(k), True),
        "y": lambda i: send_own_weight(index[i]),
        "W": lambda i, d: send_weight(index[i], int(d)),
        "f": lambda i, d: forward_weight(index[i], int(d)),
        "g": lambda i: begin(index[i]),
        "h": lambda i: have_weight(index[i]),
        "d": lambda i: queries() if i == "q" else share_rows(index[i], kb if i == "k" else vb),
        "O": send_out_weight,
        "o": lambda k: relay_out_weight(int(k)),
        "a": lambda k: attend(int(k)),
        "r": lambda d: forward_heads(int(d)),
        "P": lambda e, p: project_theirs(int(e), int(p)),
        "S": lambda e, p: project_mine(int(e), int(p)),
        "H": have_heads,
        "X": lambda e, p: add_up(int(e), int(p)),
        "F": lambda p: finished(int(p)),
        "Z": all_finished,
    }
    for name in PLAN:
        run[name[0]](*name[1:])

    for column in range(n):
        out[:, column * ocols:(column + 1) * ocols] = staged[column]
    for copy, cond in pending:
        if cond is None:
            copy.wait_send()
        else:
            pl.when(cond)(copy.wait_send)


def solution(mesh):
    n, parts = mesh.shape["sp"], mesh.shape["tp"]

    def step(tokens, query_weight, key_weight, value_weight, out_weight, mix_lambda, head_gain):
        rows, width = tokens.shape
        heads = mix_lambda.shape[0]
        vdim = head_gain.shape[0]
        groups = n // heads
        ocols = out_weight.shape[1]
        pieces = groups * heads // 2
        nbits = parts.bit_length() - 1
        dma = pltpu.SemaphoreType.DMA
        bf16 = jnp.bfloat16
        more = max(groups - 1, 1)
        chunks = 2
        vmem = pl.BlockSpec(memory_space=pltpu.VMEM)
        return pl.pallas_call(
            functools.partial(kernel, n, parts, heads),
            out_shape=jax.ShapeDtypeStruct((rows, width), bf16),
            in_specs=[vmem] * 5 + [pl.BlockSpec(memory_space=pltpu.SMEM), vmem],
            out_specs=vmem,
            scratch_shapes=[
                pltpu.VMEM((heads * rows, width), bf16),
                pltpu.VMEM((3, width, vdim), bf16),
                pltpu.VMEM((3, heads * rows, vdim), jnp.float32),
                pltpu.VMEM((heads * rows, vdim), bf16),
                pltpu.VMEM((n * rows, vdim), bf16),
                pltpu.VMEM((n * rows, vdim), bf16),
                pltpu.VMEM((heads, heads * vdim, ocols), bf16),
                pltpu.VMEM((heads, rows, vdim), bf16),
                pltpu.VMEM((groups, heads, rows, vdim), bf16),
                pltpu.VMEM((pieces, rows, ocols), bf16),
                pltpu.VMEM((pieces, rows, ocols), bf16),
                pltpu.VMEM((nbits, pieces, rows, ocols), bf16),
                pltpu.VMEM((nbits, pieces, rows, ocols), bf16),
                pltpu.VMEM((n, rows, ocols), bf16),
                dma((5,)),
                dma((heads, 2, chunks)), dma((heads, parts, chunks)), dma((heads, parts, chunks)),
                dma((heads, 3)), dma((heads, more, 3)), dma((n, 3)),
                dma((2, heads, more)), dma((2, n)),
                dma((heads, 2)), dma((heads,)),
                dma((heads,)), dma((heads,)),
                dma((more, heads)), dma((groups, heads)),
                dma((pieces,)), dma((pieces,)),
                dma((nbits, pieces)), dma((nbits, pieces)),
                dma((pieces,)), dma((n,)), dma((n,)), dma((n,)),
            ],
            compiler_params=pltpu.CompilerParams(
                collective_id=0, has_side_effects=True, vmem_limit_bytes=60000 * 1024
            ),
        )(tokens, query_weight, key_weight, value_weight, out_weight, mix_lambda,
          head_gain.reshape(1, vdim))

    placed = (
        P("sp", None),
        P("sp", "tp"),
        P("sp", "tp"),
        P("sp", "tp"),
        P("tp", "sp"),
        P("tp"),
        P(),
    )
    return jax.shard_map(step, mesh=mesh, in_specs=placed, out_specs=P("sp", None), check_vma=False)
```

```python
import functools

import jax
import jax.numpy as jnp
from jax import lax
from jax.experimental import pallas as pl
from jax.experimental.pallas import tpu as pltpu
from jax.sharding import PartitionSpec as P

MESH = pl.DeviceIdType.MESH
Q, K, V = 0, 1, 2
PLAN = (
    "t0", "yv", "Wv1", "Wk3", "t10", "fv1", "t11", "Wv3", "Wv2", "Wk1", "yq", "Wq3", "yk", "fk3",
    "t20", "fv2", "m11", "m20", "fv3", "m10", "Wk2", "fk1", "Wq1", "t21", "hv", "e1", "fq3", "m21",
    "Wq2", "fk2", "fq1", "O", "t31", "hk", "t30", "b0", "fq2", "m31", "e2", "b2", "b1", "m30", "e3",
    "b3", "gq", "o1", "hq", "dq", "a0", "a3", "a2", "a1", "r0", "r3", "o2", "r1", "r2", "P00",
    "S00", "H", "P10", "S10", "o3", "P11", "X00", "S11", "X10", "P01", "S01", "X11", "F0", "F1",
    "X01", "Z",
)


def kernel(
    n, parts, heads, chunks,
    tok, wq, wk, wv, wo_in, lam_in, gain_in, out,
    x, wown, w, acc, qb, kv, wo, ho_out, ho, part_out, part_in, sum_out, sum_in, staged, gain, lam,
    local_sem, sent, xz_recv, xx_recv, xe_recv, wz_recv, wy_recv, kv_recv, wo_recv, ho_recv,
    hof_recv, p_recv, s_recv, f_recv, d_recv,
):
    groups = n // heads
    s, t = lax.axis_index("sp"), lax.axis_index("tp")
    h, r = lax.div(s, groups), lax.rem(s, groups)
    rows, width = tok.shape
    depth = wq.shape[0]
    vdim = gain.shape[-1]
    seg = width // parts
    ocols = wo_in.shape[1]
    bits = [1 << i for i in range(parts.bit_length() - 1)]
    by_source = depth % 128 == 0
    low = lax.rem(t, 2)
    pairs = heads // 2
    chunk = rows // chunks

    def at_sp(index):
        return (index, t)

    def at_tp(index):
        return (s, index)

    def flip(index, bit):
        return index + bit - 2 * bit * lax.rem(lax.div(index, bit), 2)

    def ds(index, size):
        return pl.ds(pl.multiple_of(index * size, size), size)

    (TOKENS_Z, WEIGHTS_Z, WEIGHTS_Y, SPREAD, KEYS_Y, OUT_Z, HEADS_Z, HEADS_Y,
     PARTS, SUMS, RESULTS_Y, RESULTS) = range(12)

    def send(src, dst, kind, recv_sem, device, cond=None):
        copy = pltpu.make_async_remote_copy(
            src_ref=src, dst_ref=dst, send_sem=sent.at[kind], recv_sem=recv_sem,
            device_id=device, device_id_type=MESH,
        )
        if cond is None:
            copy.start()
        else:
            pl.when(cond)(copy.start)

    def arrived(ref, sem):
        pltpu.make_async_copy(ref, ref, sem).wait()

    barrier = pltpu.get_barrier_semaphore()
    for d in range(1, heads):
        pl.semaphore_signal(
            barrier, inc=1, device_id=at_sp(lax.rem(h + d, heads) * groups + r), device_id_type=MESH
        )
    for d in range(1, groups):
        pl.semaphore_signal(
            barrier, inc=1, device_id=at_sp(h * groups + lax.rem(r + d, groups)), device_id_type=MESH
        )
    for bit in bits:
        pl.semaphore_signal(barrier, inc=1, device_id=at_tp(flip(t, bit)), device_id_type=MESH)

    def x_at(block, part, c):
        return x.at[ds(block * chunks + c, chunk), ds(part, seg)]

    def w_at(block, i):
        return w.at[ds(block, depth), pl.ds(i * vdim, vdim)]

    right, left = at_sp(s + groups), at_sp(s - groups)
    can_right, can_left = h + 1 < heads, h > 0
    onward = ((right, can_right), (left, can_left))
    weights = (wq, wk, wv)
    peers = [at_sp(h * groups + lax.rem(r + e, groups)) for e in range(1, groups)]
    others = [lax.rem(r + e, groups) for e in range(1, groups)]

    loads = {"tok": pltpu.make_async_copy(tok, x.at[ds(h, rows), :], local_sem.at[0])}
    for i in (V, K, Q):
        loads["own", i] = pltpu.make_async_copy(weights[i], wown.at[i], local_sem.at[1 + i])
        loads["mine", i] = pltpu.make_async_copy(
            weights[i].at[:, ds(h, vdim)], w_at(s, i), local_sem.at[4 + i]
        )
    loads["out"] = pltpu.make_async_copy(wo_in, wo.at[h], local_sem.at[7])
    loads["lam"] = pltpu.make_async_copy(lam_in, lam, local_sem.at[8])
    loads["gain"] = pltpu.make_async_copy(gain_in, gain, local_sem.at[9])
    for copy in loads.values():
        copy.start()

    def loaded(key):
        if key in loads:
            loads.pop(key).wait()

    pl.semaphore_wait(barrier, heads + groups - 2 + len(bits))

    def send_tokens():
        loaded("tok")
        for c in range(chunks):
            for target, can in onward:
                send(x_at(h, t, c), x_at(h, t, c), TOKENS_Z, xz_recv.at[h, c], target, can)

    def send_own_weight(i):
        loaded(("mine", i))
        for peer in peers:
            send(w_at(s, i), w_at(s, i), WEIGHTS_Y, wy_recv.at[i], peer)

    def send_weight(i, d):
        loaded(("own", i))
        for owner, cond in ((h + d, h + d < heads), (h - d, h - d >= 0)):
            safe = jnp.where(cond, owner, h)
            send(wown.at[i, :, ds(safe, vdim)], w_at(s, i), WEIGHTS_Z, wz_recv.at[h, i],
                 at_sp(safe * groups + r), cond)

    spread = [(v, [b for b in reversed(bits) if v == 0 or b < (v & -v)]) for v in range(parts)]
    relays = [v for v, along in spread if v and along]
    leaves = parts - 1 - len(relays)

    def part_of(v):
        part = t
        for b in bits:
            if v & b:
                part = flip(part, b)
        return part

    def spread_sem(block, v, c):
        return xx_recv.at[block, relays.index(v), c] if v in relays else xe_recv.at[block]

    def pass_on(block, v, c, cond):
        piece = x_at(block, part_of(v), c)
        for b in spread[v][1]:
            send(piece, piece, SPREAD, spread_sem(block, v | b, c), at_tp(flip(t, b)), cond)

    def reach(k):
        if k == 0:
            return [(h, None, 0)]
        return [
            (jnp.where(have, block, h), have, side)
            for side, (block, have) in enumerate(((h - k, h - k >= 0), (h + k, h + k < heads)))
        ]

    def when(have, body):
        if have is None:
            body()
        else:
            pl.when(have)(body)

    def relay_tokens(k, c):
        for safe, have, side in reach(k):
            when(have, lambda safe=safe: arrived(x_at(safe, t, c), xz_recv.at[safe, c]))
            if k < heads - 1:
                target, can = onward[side]
                send(x_at(safe, t, c), x_at(safe, t, c), TOKENS_Z, xz_recv.at[safe, c], target,
                     jnp.logical_and(have, can))
            pass_on(safe, 0, c, have)

    def spread_tokens(k, c):
        for v in sorted(relays, reverse=True):
            for safe, have, _ in reach(k):
                when(have, lambda safe=safe: arrived(x_at(safe, part_of(v), c), spread_sem(safe, v, c)))
                pass_on(safe, v, c, have)

    def have_tokens(k):
        for safe, have, _ in reach(k):
            when(have, lambda safe=safe: arrived(x.at[ds(safe, rows), :leaves * seg], xe_recv.at[safe]))

    def forward_weight(i, d):
        for source_h, have, _ in reach(d):
            piece = w_at(source_h * groups + r, i)
            when(have, lambda piece=piece, source_h=source_h: arrived(piece, wz_recv.at[source_h, i]))
            for peer in peers:
                send(piece, piece, WEIGHTS_Y, wy_recv.at[i], peer, have)

    def have_weight(i):
        arrived(w.at[:(groups - 1) * heads * depth, pl.ds(i * vdim, vdim)], wy_recv.at[i])

    def begin_queries():
        loaded("tok")
        loaded(("mine", Q))
        if by_source:
            acc[...] = query_product(r)

    def query_product(group):
        total = None
        for k in range(heads):
            source = k * groups + group
            term = jnp.dot(x[:, ds(source, depth)], w[ds(source, depth), :vdim],
                           preferred_element_type=jnp.float32)
            total = term if total is None else total + term
        return total

    def finish_queries():
        if not by_source:
            full = jnp.dot(x[...], w[:, :vdim], preferred_element_type=jnp.float32)
        else:
            full = acc[...]
            for other in others:
                full = full + query_product(other)
        qb[...] = full.astype(jnp.bfloat16)

    def share_rows(k):
        loaded("tok")
        loaded(("mine", K))
        loaded(("mine", V))

        def body(block):
            mine = ds(block * groups + r, rows)
            kv[mine, :] = jnp.dot(
                x[ds(block, rows), :], w[:, vdim:], preferred_element_type=jnp.float32
            ).astype(jnp.bfloat16)
            for peer in peers:
                send(kv.at[mine, :], kv.at[mine, :], KEYS_Y, kv_recv.at[block], peer)

        for safe, have, _ in reach(k):
            when(have, lambda safe=safe: body(safe))

    def send_out_weight():
        loaded("out")
        for target, can in onward:
            send(wo.at[h], wo.at[h], OUT_Z, wo_recv.at[h], target, can)

    def relay_out_weight(k):
        for safe, have, side in reach(k):
            when(have, lambda safe=safe: arrived(wo.at[safe], wo_recv.at[safe]))
            if k < heads - 1:
                target, can = onward[side]
                send(wo.at[safe], wo.at[safe], OUT_Z, wo_recv.at[safe], target,
                     jnp.logical_and(have, can))

    lane = lax.broadcasted_iota(jnp.int32, (rows, vdim), 1)
    factor = (vdim // 2) ** (-0.5) * 1.4426950408889634
    seen = []

    def attend(k):
        for j in range(k + 1):
            if j not in seen:
                seen.append(j)
                arrived(kv.at[:(groups - 1) * rows, :], kv_recv.at[j])
        loaded("lam")
        loaded("gain")
        lam_here = jnp.float32(0.0)
        for j in range(heads):
            lam_here = jnp.where(h == j, lam[j], lam_here)
        extent = (k + 1) * groups * rows
        q_rows = qb[k * rows:(k + 1) * rows, :]
        keys = kv[:extent, :vdim]
        values = kv[:extent, vdim:]
        ahead = lax.broadcasted_iota(jnp.int32, (rows, extent), 1) - lax.broadcasted_iota(
            jnp.int32, (rows, extent), 0
        )
        visible = ahead <= (k * groups + r) * rows
        maps = []
        for c in range(2):
            picked = jnp.where((lane >= vdim // 2) == (c == 1), q_rows, jnp.zeros_like(q_rows))
            scores = lax.dot_general(
                picked, keys, (((1,), (1,)), ((), ())), preferred_element_type=jnp.float32
            )
            scores = jnp.where(visible, scores, -1e30)
            top = jnp.max(scores, axis=-1, keepdims=True)
            e = jnp.exp2((scores - top) * factor)
            total = jnp.sum(e, axis=-1, keepdims=True)
            mixed = jnp.dot(e.astype(jnp.bfloat16), values, preferred_element_type=jnp.float32)
            maps.append(mixed / total)
        mixture = maps[0] - lam_here * maps[1]
        normalized = (
            mixture
            * lax.rsqrt(jnp.mean(mixture * mixture, axis=-1, keepdims=True) + 1e-05)
            * gain[...]
        )
        ho_out[k] = normalized.astype(jnp.bfloat16)
        send(ho_out.at[k], ho.at[r, h], HEADS_Z, ho_recv.at[h], at_sp(k * groups + r), k != h)

        @pl.when(k == h)
        def _():
            ho[r, h] = ho_out[k]

    def forward_heads(d):
        for source, have, _ in reach(d):
            if d:
                when(have, lambda source=source: arrived(ho.at[r, source], ho_recv.at[source]))
            for peer in peers:
                send(ho.at[r, source], ho.at[r, source], HEADS_Y, hof_recv.at[0], peer, have)

    def have_heads():
        arrived(ho.at[:groups - 1], hof_recv.at[0])

    buddy = at_tp(flip(t, 1))
    members = [r] + others

    def column_block(p, which):
        return 2 * lax.rem(lax.div(h, 2) + p, pairs) + lax.rem(h + which, 2)

    def which_rows(later):
        return range(1, groups) if later else range(1)

    def partial_product(e, p, which):
        lhs = jnp.concatenate([ho[members[e], k] for k in range(heads)], axis=-1)
        return jnp.dot(lhs, wo[column_block(p, which)], preferred_element_type=jnp.float32)

    def project_theirs(later, p):
        for e in which_rows(later):
            j = e * pairs + p
            part_out[j] = partial_product(e, p, 1 - low).astype(jnp.bfloat16)
            send(part_out.at[j], part_in.at[j], PARTS, p_recv.at[j], buddy)

    def project_mine(later, p):
        for e in which_rows(later):
            j = e * pairs + p
            own = partial_product(e, p, low)
            arrived(part_in.at[j], p_recv.at[j])
            sum_out[0, j] = (own + part_in[j].astype(jnp.float32)).astype(jnp.bfloat16)
            send(sum_out.at[0, j], sum_in.at[0, j], SUMS, s_recv.at[0, j], at_tp(flip(t, bits[1])))

    def add_up(later, p):
        last = len(bits) - 1
        for e in which_rows(later):
            j = e * pairs + p
            for i in range(1, len(bits)):
                arrived(sum_in.at[i - 1, j], s_recv.at[i - 1, j])
                total = (
                    sum_out[i - 1, j].astype(jnp.float32) + sum_in[i - 1, j].astype(jnp.float32)
                ).astype(jnp.bfloat16)
                if i < last:
                    sum_out[i, j] = total
                    send(sum_out.at[i, j], sum_in.at[i, j], SUMS, s_recv.at[i, j],
                         at_tp(flip(t, bits[i + 1])))
            column = column_block(p, low) * groups + r
            if e == 0:
                staged[column] = total
                send(staged.at[column], staged.at[column], RESULTS, d_recv.at[0], buddy)
            else:
                sum_out[last, j] = total
                send(sum_out.at[last, j], staged.at[column], RESULTS_Y, f_recv.at[r, p], peers[e - 1])

    def finished(p):
        for other in others:
            column = column_block(p, low) * groups + other
            arrived(staged.at[column], f_recv.at[other, p])
            send(staged.at[column], staged.at[column], RESULTS, d_recv.at[0], buddy)

    def all_finished():
        arrived(part_in, d_recv.at[0])

    index = {"q": Q, "k": K, "v": V}
    run = {
        "t": lambda k, c=0: relay_tokens(int(k), int(c)) if int(k) else send_tokens(),
        "m": lambda k, c: spread_tokens(int(k), int(c)),
        "e": lambda k: have_tokens(int(k)),
        "y": lambda i: send_own_weight(index[i]),
        "W": lambda i, d: send_weight(index[i], int(d)),
        "f": lambda i, d: forward_weight(index[i], int(d)),
        "h": lambda i: have_weight(index[i]),
        "b": lambda k: share_rows(int(k)),
        "g": lambda i: begin_queries(),
        "d": lambda i: finish_queries(),
        "O": send_out_weight,
        "o": lambda k: relay_out_weight(int(k)),
        "a": lambda k: attend(int(k)),
        "r": lambda d: forward_heads(int(d)),
        "P": lambda e, p: project_theirs(int(e), int(p)),
        "S": lambda e, p: project_mine(int(e), int(p)),
        "H": have_heads,
        "X": lambda e, p: add_up(int(e), int(p)),
        "F": lambda p: finished(int(p)),
        "Z": all_finished,
    }
    for name in PLAN:
        run[name[0]](*name[1:])

    for column in range(n):
        out[:, column * ocols:(column + 1) * ocols] = staged[column]
    inner = jnp.logical_and(can_right, can_left)
    blocks = heads + 1
    out_rows = blocks * heads * vdim * ocols // width
    pl.when(inner)(lambda: arrived(x.at[:, :blocks * seg // heads], sent.at[TOKENS_Z]))
    pl.when(jnp.logical_not(inner))(lambda: arrived(x.at[:rows, :seg], sent.at[TOKENS_Z]))
    pl.when(inner)(lambda: arrived(x.at[:out_rows, :], sent.at[OUT_Z]))
    pl.when(jnp.logical_not(inner))(lambda: arrived(wo.at[0], sent.at[OUT_Z]))
    arrived(wown.at[:, :, :(heads - 1) * vdim], sent.at[WEIGHTS_Z])
    arrived(w.at[:(groups - 1) * heads * depth, :], sent.at[WEIGHTS_Y])
    arrived(x.at[:, :(heads - 1) * (parts - 1) * seg // heads], sent.at[SPREAD])
    arrived(kv.at[:heads * (groups - 1) * rows, :], sent.at[KEYS_Y])
    arrived(ho_out.at[:heads - 1], sent.at[HEADS_Z])
    arrived(ho.at[:groups - 1], sent.at[HEADS_Y])
    arrived(part_out, sent.at[PARTS])
    arrived(sum_out.at[:len(bits) - 1], sent.at[SUMS])
    arrived(part_out.at[:(groups - 1) * pairs], sent.at[RESULTS_Y])
    arrived(part_out, sent.at[RESULTS])


def solution(mesh):
    n, parts = mesh.shape["sp"], mesh.shape["tp"]

    def step(tokens, query_weight, key_weight, value_weight, out_weight, mix_lambda, head_gain):
        rows, width = tokens.shape
        heads = mix_lambda.shape[0]
        vdim = head_gain.shape[0]
        depth = query_weight.shape[0]
        groups = n // heads
        ocols = out_weight.shape[1]
        pairs = heads // 2
        pieces = groups * pairs
        nbits = parts.bit_length() - 1
        chunks = 2
        dma = pltpu.SemaphoreType.DMA
        bf16 = jnp.bfloat16
        limit = 32 * 1024 if n * rows <= 2048 else 60000
        operands = [pltpu.with_memory_space_constraint(operand, pltpu.HBM) for operand in (
            tokens, query_weight, key_weight, value_weight, out_weight, mix_lambda,
            head_gain.reshape(1, vdim),
        )]
        return pl.pallas_call(
            functools.partial(kernel, n, parts, heads, chunks),
            out_shape=pltpu.VMEM((rows, width), bf16),
            in_specs=[pl.BlockSpec(memory_space=pltpu.HBM)] * 7,
            out_specs=pl.BlockSpec(memory_space=pltpu.VMEM),
            scratch_shapes=[
                pltpu.VMEM((heads * rows, width), bf16),
                pltpu.VMEM((3, depth, heads * vdim), bf16),
                pltpu.VMEM((width, 3 * vdim), bf16),
                pltpu.VMEM((heads * rows, vdim), jnp.float32),
                pltpu.VMEM((heads * rows, vdim), bf16),
                pltpu.VMEM((n * rows, 2 * vdim), bf16),
                pltpu.VMEM((heads, heads * vdim, ocols), bf16),
                pltpu.VMEM((heads, rows, vdim), bf16),
                pltpu.VMEM((groups, heads, rows, vdim), bf16),
                pltpu.VMEM((pieces, rows, ocols), bf16),
                pltpu.VMEM((pieces, rows, ocols), bf16),
                pltpu.VMEM((nbits, pieces, rows, ocols), bf16),
                pltpu.VMEM((nbits, pieces, rows, ocols), bf16),
                pltpu.VMEM((n, rows, ocols), bf16),
                pltpu.VMEM((1, vdim), jnp.float32),
                pltpu.SMEM((heads,), jnp.float32),
                dma((10,)), dma((12,)),
                dma((heads, chunks)), dma((heads, parts // 2 - 1, chunks)), dma((heads,)),
                dma((heads, 3)), dma((3,)), dma((heads,)), dma((heads,)), dma((heads,)),
                dma((1,)), dma((pieces,)), dma((nbits - 1, pieces)), dma((groups, pairs)), dma((1,)),
            ],
            compiler_params=pltpu.CompilerParams(
                collective_id=0, has_side_effects=True, vmem_limit_bytes=limit * 1024
            ),
        )(*operands)

    placed = (
        P("sp", None),
        P("sp", "tp"),
        P("sp", "tp"),
        P("sp", "tp"),
        P("tp", "sp"),
        P("tp"),
        P(),
    )
    return jax.shard_map(step, mesh=mesh, in_specs=placed, out_specs=P("sp", None), check_vma=False)
```

```python
import functools

import jax
import jax.numpy as jnp
from jax import lax
from jax.experimental import pallas as pl
from jax.experimental.pallas import tpu as pltpu
from jax.sharding import PartitionSpec as P

MESH = pl.DeviceIdType.MESH
Q, K, V = 0, 1, 2
PLAN = (
    "yq", "yk", "yv", "t0", "Wk3", "Wv1", "Wv3", "t11", "Wv2", "t10", "Wq3", "Wq1", "Wk1", "t21",
    "fv3", "fv1", "fv2", "m10", "t20", "m11", "fq1", "Wk2", "m20", "t31", "hv", "e1", "m21", "Wq2",
    "fq3", "fk3", "fk1", "fk2", "O0", "O1", "t30", "fq2", "hk", "m31", "e2", "b0", "m30", "b1",
    "e3", "gq", "b3", "o10", "o11", "hq", "b2", "dq", "a0", "a1", "a3", "a2", "o20", "o21", "r0",
    "r1", "r2", "r3", "P00", "P01", "S00", "S01", "H", "P10", "P11", "S10", "S11", "X00", "X01",
    "o30", "o31", "P12", "P13", "S12", "S13", "X10", "X11", "P02", "P03", "S02", "S03", "X12",
    "X13", "X02", "X03", "F0", "F1", "F2", "F3", "Z",
)


def kernel(
    n, parts, heads, chunks,
    tok, wq, wk, wv, wo_in, lam_in, gain_in, out,
    x, wown, w, acc, qb, kv, wo, ho_out, ho, part_out, part_in, sum_out, sum_in, staged, gain, lam,
    local_sem, sent, xz_recv, xx_recv, xe_recv, wz_recv, wy_recv, kv_recv, wo_recv, ho_recv,
    hof_recv, p_recv, s_recv, f_recv, d_recv,
):
    groups = n // heads
    s, t = lax.axis_index("sp"), lax.axis_index("tp")
    h, r = lax.div(s, groups), lax.rem(s, groups)
    rows, width = tok.shape
    depth = wq.shape[0]
    vdim = gain.shape[-1]
    seg = width // parts
    ocols = wo_in.shape[1]
    bits = [1 << i for i in range(parts.bit_length() - 1)]
    by_source = depth % 128 == 0
    low = lax.rem(t, 2)
    pairs = heads // 2
    chunk = rows // chunks
    halves = wo.shape[0] // heads
    hcols = ocols // halves

    def at_sp(index):
        return (index, t)

    def at_tp(index):
        return (s, index)

    def flip(index, bit):
        return index + bit - 2 * bit * lax.rem(lax.div(index, bit), 2)

    def ds(index, size):
        return pl.ds(pl.multiple_of(index * size, size), size)

    (TOKENS_Z, WEIGHTS_Z, WEIGHTS_Y, SPREAD, KEYS_Y, OUT_Z, HEADS_Z, HEADS_Y,
     PARTS, SUMS, RESULTS_Y, RESULTS) = range(12)

    def send(src, dst, kind, recv_sem, device, cond=None):
        copy = pltpu.make_async_remote_copy(
            src_ref=src, dst_ref=dst, send_sem=sent.at[kind], recv_sem=recv_sem,
            device_id=device, device_id_type=MESH,
        )
        if cond is None:
            copy.start()
        else:
            pl.when(cond)(copy.start)

    def arrived(ref, sem):
        pltpu.make_async_copy(ref, ref, sem).wait()

    barrier = pltpu.get_barrier_semaphore()
    for d in range(1, heads):
        pl.semaphore_signal(
            barrier, inc=1, device_id=at_sp(lax.rem(h + d, heads) * groups + r), device_id_type=MESH
        )
    for d in range(1, groups):
        pl.semaphore_signal(
            barrier, inc=1, device_id=at_sp(h * groups + lax.rem(r + d, groups)), device_id_type=MESH
        )
    for bit in bits:
        pl.semaphore_signal(barrier, inc=1, device_id=at_tp(flip(t, bit)), device_id_type=MESH)

    def x_at(block, part, c):
        return x.at[ds(block * chunks + c, chunk), ds(part, seg)]

    def w_at(block, i):
        return w.at[ds(block, depth), pl.ds(i * vdim, vdim)]

    right, left = at_sp(s + groups), at_sp(s - groups)
    can_right, can_left = h + 1 < heads, h > 0
    onward = ((right, can_right), (left, can_left))
    weights = (wq, wk, wv)
    peers = [at_sp(h * groups + lax.rem(r + e, groups)) for e in range(1, groups)]
    others = [lax.rem(r + e, groups) for e in range(1, groups)]

    loads = {"tok": pltpu.make_async_copy(tok, x.at[ds(h, rows), :], local_sem.at[0])}
    for i in (V, K, Q):
        loads["own", i] = pltpu.make_async_copy(weights[i], wown.at[i], local_sem.at[1 + i])
        loads["mine", i] = pltpu.make_async_copy(
            weights[i].at[:, ds(h, vdim)], w_at(s, i), local_sem.at[4 + i]
        )
    loads["lam"] = pltpu.make_async_copy(lam_in, lam, local_sem.at[7])
    loads["gain"] = pltpu.make_async_copy(gain_in, gain, local_sem.at[8])
    for c in range(halves):
        loads["out", c] = pltpu.make_async_copy(
            wo_in.at[:, pl.ds(c * hcols, hcols)], wo.at[h * halves + c], local_sem.at[9 + c]
        )
    for copy in loads.values():
        copy.start()

    def loaded(key):
        if key in loads:
            loads.pop(key).wait()

    pl.semaphore_wait(barrier, heads + groups - 2 + len(bits))

    def send_tokens():
        loaded("tok")
        for c in range(chunks):
            for target, can in onward:
                send(x_at(h, t, c), x_at(h, t, c), TOKENS_Z, xz_recv.at[h, c], target, can)

    def send_own_weight(i):
        loaded(("mine", i))
        for peer in peers:
            send(w_at(s, i), w_at(s, i), WEIGHTS_Y, wy_recv.at[i], peer)

    def send_weight(i, d):
        loaded(("own", i))
        for owner, cond in ((h + d, h + d < heads), (h - d, h - d >= 0)):
            safe = jnp.where(cond, owner, h)
            send(wown.at[i, :, ds(safe, vdim)], w_at(s, i), WEIGHTS_Z, wz_recv.at[h, i],
                 at_sp(safe * groups + r), cond)

    spread = [(v, [b for b in reversed(bits) if v == 0 or b < (v & -v)]) for v in range(parts)]
    relays = [v for v, along in spread if v and along]
    leaves = parts - 1 - len(relays)

    def part_of(v):
        part = t
        for b in bits:
            if v & b:
                part = flip(part, b)
        return part

    def spread_sem(block, v, c):
        return xx_recv.at[block, relays.index(v), c] if v in relays else xe_recv.at[block]

    def pass_on(block, v, c, cond):
        piece = x_at(block, part_of(v), c)
        for b in spread[v][1]:
            send(piece, piece, SPREAD, spread_sem(block, v | b, c), at_tp(flip(t, b)), cond)

    def reach(k):
        if k == 0:
            return [(h, None, 0)]
        return [
            (jnp.where(have, block, h), have, side)
            for side, (block, have) in enumerate(((h - k, h - k >= 0), (h + k, h + k < heads)))
        ]

    def when(have, body):
        if have is None:
            body()
        else:
            pl.when(have)(body)

    def relay_tokens(k, c):
        for safe, have, side in reach(k):
            when(have, lambda safe=safe: arrived(x_at(safe, t, c), xz_recv.at[safe, c]))
            if k < heads - 1:
                target, can = onward[side]
                send(x_at(safe, t, c), x_at(safe, t, c), TOKENS_Z, xz_recv.at[safe, c], target,
                     jnp.logical_and(have, can))
            pass_on(safe, 0, c, have)

    def spread_tokens(k, c):
        for v in sorted(relays, reverse=True):
            for safe, have, _ in reach(k):
                when(have, lambda safe=safe: arrived(x_at(safe, part_of(v), c), spread_sem(safe, v, c)))
                pass_on(safe, v, c, have)

    def have_tokens(k):
        for safe, have, _ in reach(k):
            when(have, lambda safe=safe: arrived(x.at[ds(safe, rows), :leaves * seg], xe_recv.at[safe]))

    def forward_weight(i, d):
        for source_h, have, _ in reach(d):
            piece = w_at(source_h * groups + r, i)
            when(have, lambda piece=piece, source_h=source_h: arrived(piece, wz_recv.at[source_h, i]))
            for peer in peers:
                send(piece, piece, WEIGHTS_Y, wy_recv.at[i], peer, have)

    def have_weight(i):
        arrived(w.at[:(groups - 1) * heads * depth, pl.ds(i * vdim, vdim)], wy_recv.at[i])

    def begin_queries():
        loaded("tok")
        loaded(("mine", Q))
        if by_source:
            acc[...] = query_product(r)

    def query_product(group):
        total = None
        for k in range(heads):
            source = k * groups + group
            term = jnp.dot(x[:, ds(source, depth)], w[ds(source, depth), :vdim],
                           preferred_element_type=jnp.float32)
            total = term if total is None else total + term
        return total

    def finish_queries():
        if not by_source:
            full = jnp.dot(x[...], w[:, :vdim], preferred_element_type=jnp.float32)
        else:
            full = acc[...]
            for other in others:
                full = full + query_product(other)
        qb[...] = full.astype(jnp.bfloat16)

    def share_rows(k):
        loaded("tok")
        loaded(("mine", K))
        loaded(("mine", V))

        def body(block):
            mine = ds(block * groups + r, rows)
            kv[mine, :] = jnp.dot(
                x[ds(block, rows), :], w[:, vdim:], preferred_element_type=jnp.float32
            ).astype(jnp.bfloat16)
            for peer in peers:
                send(kv.at[mine, :], kv.at[mine, :], KEYS_Y, kv_recv.at[block], peer)

        for safe, have, _ in reach(k):
            when(have, lambda safe=safe: body(safe))

    def send_out_weight(c):
        if c >= halves:
            return
        loaded(("out", c))
        piece = h * halves + c
        for target, can in onward:
            send(wo.at[piece], wo.at[piece], OUT_Z, wo_recv.at[piece], target, can)

    def relay_out_weight(k, c):
        if c >= halves:
            return
        for safe, have, side in reach(k):
            piece = safe * halves + c
            when(have, lambda piece=piece: arrived(wo.at[piece], wo_recv.at[piece]))
            if k < heads - 1:
                target, can = onward[side]
                send(wo.at[piece], wo.at[piece], OUT_Z, wo_recv.at[piece], target,
                     jnp.logical_and(have, can))

    lane = lax.broadcasted_iota(jnp.int32, (rows, vdim), 1)
    factor = (vdim // 2) ** (-0.5) * 1.4426950408889634
    seen = []

    def attend(k):
        for j in range(k + 1):
            if j not in seen:
                seen.append(j)
                arrived(kv.at[:(groups - 1) * rows, :], kv_recv.at[j])
        loaded("lam")
        loaded("gain")
        lam_here = jnp.float32(0.0)
        for j in range(heads):
            lam_here = jnp.where(h == j, lam[j], lam_here)
        extent = (k + 1) * groups * rows
        q_rows = qb[k * rows:(k + 1) * rows, :]
        keys = kv[:extent, :vdim]
        values = kv[:extent, vdim:]
        ahead = lax.broadcasted_iota(jnp.int32, (rows, extent), 1) - lax.broadcasted_iota(
            jnp.int32, (rows, extent), 0
        )
        visible = ahead <= (k * groups + r) * rows
        maps = []
        for c in range(2):
            picked = jnp.where((lane >= vdim // 2) == (c == 1), q_rows, jnp.zeros_like(q_rows))
            scores = lax.dot_general(
                picked, keys, (((1,), (1,)), ((), ())), preferred_element_type=jnp.float32
            )
            scores = jnp.where(visible, scores, -1e30)
            top = jnp.max(scores, axis=-1, keepdims=True)
            e = jnp.exp2((scores - top) * factor)
            total = jnp.sum(e, axis=-1, keepdims=True)
            mixed = jnp.dot(e.astype(jnp.bfloat16), values, preferred_element_type=jnp.float32)
            maps.append(mixed / total)
        mixture = maps[0] - lam_here * maps[1]
        normalized = (
            mixture
            * lax.rsqrt(jnp.mean(mixture * mixture, axis=-1, keepdims=True) + 1e-05)
            * gain[...]
        )
        ho_out[k] = normalized.astype(jnp.bfloat16)
        send(ho_out.at[k], ho.at[r, h], HEADS_Z, ho_recv.at[h], at_sp(k * groups + r), k != h)

        @pl.when(k == h)
        def _():
            ho[r, h] = ho_out[k]

    def forward_heads(d):
        for source, have, _ in reach(d):
            if d:
                when(have, lambda source=source: arrived(ho.at[r, source], ho_recv.at[source]))
            for peer in peers:
                send(ho.at[r, source], ho.at[r, source], HEADS_Y, hof_recv.at[0], peer, have)

    def have_heads():
        arrived(ho.at[:groups - 1], hof_recv.at[0])

    buddy = at_tp(flip(t, 1))
    members = [r] + others

    def column_block(pair, which):
        return 2 * lax.rem(lax.div(h, 2) + pair, pairs) + lax.rem(h + which, 2)

    def pieces_of(later, p):
        pair, half = p // 2, p % 2
        if half >= halves:
            return []
        return [
            (e, pair, half, (e * pairs + pair) * halves + half)
            for e in (range(1, groups) if later else range(1))
        ]

    def partial_product(e, pair, half, which):
        lhs = jnp.concatenate([ho[members[e], k] for k in range(heads)], axis=-1)
        return jnp.dot(lhs, wo[column_block(pair, which) * halves + half],
                       preferred_element_type=jnp.float32)

    def project_theirs(later, p):
        for e, pair, half, j in pieces_of(later, p):
            part_out[j] = partial_product(e, pair, half, 1 - low).astype(jnp.bfloat16)
            send(part_out.at[j], part_in.at[j], PARTS, p_recv.at[j], buddy)

    def project_mine(later, p):
        for e, pair, half, j in pieces_of(later, p):
            own = partial_product(e, pair, half, low)
            arrived(part_in.at[j], p_recv.at[j])
            sum_out[0, j] = (own + part_in[j].astype(jnp.float32)).astype(jnp.bfloat16)
            send(sum_out.at[0, j], sum_in.at[0, j], SUMS, s_recv.at[0, j], at_tp(flip(t, bits[1])))

    def add_up(later, p):
        last = len(bits) - 1
        for e, pair, half, j in pieces_of(later, p):
            for i in range(1, len(bits)):
                arrived(sum_in.at[i - 1, j], s_recv.at[i - 1, j])
                total = (
                    sum_out[i - 1, j].astype(jnp.float32) + sum_in[i - 1, j].astype(jnp.float32)
                ).astype(jnp.bfloat16)
                if i < last:
                    sum_out[i, j] = total
                    send(sum_out.at[i, j], sum_in.at[i, j], SUMS, s_recv.at[i, j],
                         at_tp(flip(t, bits[i + 1])))
            place = (column_block(pair, low) * groups + r) * halves + half
            if e == 0:
                staged[place] = total
                send(staged.at[place], staged.at[place], RESULTS, d_recv.at[0], buddy)
            else:
                sum_out[last, j] = total
                send(sum_out.at[last, j], staged.at[place], RESULTS_Y, f_recv.at[r, p], peers[e - 1])

    def finished(p):
        for e, pair, half, _ in pieces_of(True, p):
            place = (column_block(pair, low) * groups + members[e]) * halves + half
            arrived(staged.at[place], f_recv.at[members[e], p])
            send(staged.at[place], staged.at[place], RESULTS, d_recv.at[0], buddy)

    def all_finished():
        arrived(part_in, d_recv.at[0])

    index = {"q": Q, "k": K, "v": V}
    run = {
        "t": lambda k, c=0: relay_tokens(int(k), int(c)) if int(k) else send_tokens(),
        "m": lambda k, c: spread_tokens(int(k), int(c)),
        "e": lambda k: have_tokens(int(k)),
        "y": lambda i: send_own_weight(index[i]),
        "W": lambda i, d: send_weight(index[i], int(d)),
        "f": lambda i, d: forward_weight(index[i], int(d)),
        "h": lambda i: have_weight(index[i]),
        "b": lambda k: share_rows(int(k)),
        "g": lambda i: begin_queries(),
        "d": lambda i: finish_queries(),
        "O": lambda c: send_out_weight(int(c)),
        "o": lambda k, c: relay_out_weight(int(k), int(c)),
        "a": lambda k: attend(int(k)),
        "r": lambda d: forward_heads(int(d)),
        "P": lambda e, p: project_theirs(int(e), int(p)),
        "S": lambda e, p: project_mine(int(e), int(p)),
        "H": have_heads,
        "X": lambda e, p: add_up(int(e), int(p)),
        "F": lambda p: finished(int(p)),
        "Z": all_finished,
    }
    for name in PLAN:
        run[name[0]](*name[1:])

    for place in range(n * halves):
        out[:, place * hcols:(place + 1) * hcols] = staged[place]
    inner = jnp.logical_and(can_right, can_left)
    blocks = heads + 1
    out_rows = blocks * heads * vdim * ocols // width
    pl.when(inner)(lambda: arrived(x.at[:, :blocks * seg // heads], sent.at[TOKENS_Z]))
    pl.when(jnp.logical_not(inner))(lambda: arrived(x.at[:rows, :seg], sent.at[TOKENS_Z]))
    pl.when(inner)(lambda: arrived(x.at[:out_rows, :], sent.at[OUT_Z]))
    pl.when(jnp.logical_not(inner))(lambda: arrived(wo.at[:halves], sent.at[OUT_Z]))
    arrived(wown.at[:, :, :(heads - 1) * vdim], sent.at[WEIGHTS_Z])
    arrived(w.at[:(groups - 1) * heads * depth, :], sent.at[WEIGHTS_Y])
    arrived(x.at[:, :(heads - 1) * (parts - 1) * seg // heads], sent.at[SPREAD])
    arrived(kv.at[:heads * (groups - 1) * rows, :], sent.at[KEYS_Y])
    arrived(ho_out.at[:heads - 1], sent.at[HEADS_Z])
    arrived(ho.at[:groups - 1], sent.at[HEADS_Y])
    arrived(part_out, sent.at[PARTS])
    arrived(sum_out.at[:len(bits) - 1], sent.at[SUMS])
    arrived(part_out.at[:(groups - 1) * pairs * halves], sent.at[RESULTS_Y])
    arrived(part_out, sent.at[RESULTS])


def solution(mesh):
    n, parts = mesh.shape["sp"], mesh.shape["tp"]

    def step(tokens, query_weight, key_weight, value_weight, out_weight, mix_lambda, head_gain):
        rows, width = tokens.shape
        heads = mix_lambda.shape[0]
        vdim = head_gain.shape[0]
        depth = query_weight.shape[0]
        groups = n // heads
        ocols = out_weight.shape[1]
        pairs = heads // 2
        halves = 2 if ocols % 256 == 0 else 1
        hcols = ocols // halves
        pieces = groups * pairs * halves
        nbits = parts.bit_length() - 1
        chunks = 2
        dma = pltpu.SemaphoreType.DMA
        bf16 = jnp.bfloat16
        limit = 32 * 1024 if n * rows <= 2048 else 60000
        operands = [pltpu.with_memory_space_constraint(operand, pltpu.HBM) for operand in (
            tokens, query_weight, key_weight, value_weight, out_weight, mix_lambda,
            head_gain.reshape(1, vdim),
        )]
        return pl.pallas_call(
            functools.partial(kernel, n, parts, heads, chunks),
            out_shape=pltpu.VMEM((rows, width), bf16),
            in_specs=[pl.BlockSpec(memory_space=pltpu.HBM)] * 7,
            out_specs=pl.BlockSpec(memory_space=pltpu.VMEM),
            scratch_shapes=[
                pltpu.VMEM((heads * rows, width), bf16),
                pltpu.VMEM((3, depth, heads * vdim), bf16),
                pltpu.VMEM((width, 3 * vdim), bf16),
                pltpu.VMEM((heads * rows, vdim), jnp.float32),
                pltpu.VMEM((heads * rows, vdim), bf16),
                pltpu.VMEM((n * rows, 2 * vdim), bf16),
                pltpu.VMEM((heads * halves, heads * vdim, hcols), bf16),
                pltpu.VMEM((heads, rows, vdim), bf16),
                pltpu.VMEM((groups, heads, rows, vdim), bf16),
                pltpu.VMEM((pieces, rows, hcols), bf16),
                pltpu.VMEM((pieces, rows, hcols), bf16),
                pltpu.VMEM((nbits, pieces, rows, hcols), bf16),
                pltpu.VMEM((nbits, pieces, rows, hcols), bf16),
                pltpu.VMEM((n * halves, rows, hcols), bf16),
                pltpu.VMEM((1, vdim), jnp.float32),
                pltpu.SMEM((heads,), jnp.float32),
                dma((11,)), dma((12,)),
                dma((heads, chunks)), dma((heads, parts // 2 - 1, chunks)), dma((heads,)),
                dma((heads, 3)), dma((3,)), dma((heads,)), dma((heads * halves,)), dma((heads,)),
                dma((1,)), dma((pieces,)), dma((nbits - 1, pieces)), dma((groups, pairs * 2)), dma((1,)),
            ],
            compiler_params=pltpu.CompilerParams(
                collective_id=0, has_side_effects=True, vmem_limit_bytes=limit * 1024
            ),
        )(*operands)

    placed = (
        P("sp", None),
        P("sp", "tp"),
        P("sp", "tp"),
        P("sp", "tp"),
        P("tp", "sp"),
        P("tp"),
        P(),
    )
    return jax.shard_map(step, mesh=mesh, in_specs=placed, out_specs=P("sp", None), check_vma=False)
```

```python
import functools

import jax
import jax.numpy as jnp
from jax import lax
from jax.experimental import pallas as pl
from jax.experimental.pallas import tpu as pltpu
from jax.sharding import PartitionSpec as P

MESH = pl.DeviceIdType.MESH
Q, K, V = 0, 1, 2
PLAN = (
    "yq", "yk", "yv", "t0", "Wk3", "Wv1", "Wv3", "t11", "Wv2", "t10", "Wq3", "Wq1", "Wk1", "t21",
    "fv3", "fv1", "fv2", "m10", "t20", "m11", "fq1", "Wk2", "m20", "t31", "hv", "e1", "m21", "Wq2",
    "fq3", "fk3", "fk1", "fk2", "O0", "O1", "t30", "fq2", "hk", "m31", "e2", "b0", "m30", "b1",
    "e3", "gq", "b3", "b2", "o10", "o11", "hq", "dq", "a0", "a1", "a3", "a2", "o20", "o21", "r0",
    "r1", "r2", "r3", "P00", "P01", "S00", "S01", "H", "P10", "P11", "S10", "S11", "X00", "X01",
    "o30", "P12", "o31", "P13", "P02", "P03", "S12", "S13", "X10", "X11", "S02", "S03", "X12",
    "X13", "F0", "F1", "X02", "X03", "F2", "F3", "Z",
)


def kernel(
    n, parts, heads, chunks,
    tok, wq, wk, wv, wo_in, lam_in, gain_in, out,
    x, wown, w, acc, qb, kv, wo, ho_out, ho, part_out, part_in, sum_out, sum_in, staged, gain, lam,
    local_sem, sent, xz_recv, xx_recv, xe_recv, wz_recv, wy_recv, kv_recv, wo_recv, ho_recv,
    hof_recv, p_recv, s_recv, f_recv, d_recv,
):
    groups = n // heads
    s, t = lax.axis_index("sp"), lax.axis_index("tp")
    h, r = lax.div(s, groups), lax.rem(s, groups)
    rows, width = tok.shape
    depth = wq.shape[0]
    vdim = gain.shape[-1]
    seg = width // parts
    ocols = wo_in.shape[1]
    bits = [1 << i for i in range(parts.bit_length() - 1)]
    by_source = depth % 128 == 0
    low = lax.rem(t, 2)
    pairs = heads // 2
    chunk = rows // chunks
    halves = wo.shape[0] // heads
    hcols = ocols // halves

    def at_sp(index):
        return (index, t)

    def at_tp(index):
        return (s, index)

    def flip(index, bit):
        return index + bit - 2 * bit * lax.rem(lax.div(index, bit), 2)

    def ds(index, size):
        return pl.ds(pl.multiple_of(index * size, size), size)

    (TOKENS_Z, WEIGHTS_Z, WEIGHTS_Y, SPREAD, KEYS_Y, OUT_Z, HEADS_Z, HEADS_Y,
     PARTS, SUMS, RESULTS_Y, RESULTS) = range(12)

    def send(src, dst, kind, recv_sem, device, cond=None):
        copy = pltpu.make_async_remote_copy(
            src_ref=src, dst_ref=dst, send_sem=sent.at[kind], recv_sem=recv_sem,
            device_id=device, device_id_type=MESH,
        )
        if cond is None:
            copy.start()
        else:
            pl.when(cond)(copy.start)

    def arrived(ref, sem):
        pltpu.make_async_copy(ref, ref, sem).wait()

    barrier = pltpu.get_barrier_semaphore()
    for d in range(1, heads):
        pl.semaphore_signal(
            barrier, inc=1, device_id=at_sp(lax.rem(h + d, heads) * groups + r), device_id_type=MESH
        )
    for d in range(1, groups):
        pl.semaphore_signal(
            barrier, inc=1, device_id=at_sp(h * groups + lax.rem(r + d, groups)), device_id_type=MESH
        )
    for bit in bits:
        pl.semaphore_signal(barrier, inc=1, device_id=at_tp(flip(t, bit)), device_id_type=MESH)

    def x_at(block, part, c):
        return x.at[ds(block * chunks + c, chunk), ds(part, seg)]

    def w_at(block, i):
        return w.at[ds(block, depth), pl.ds(i * vdim, vdim)]

    right, left = at_sp(s + groups), at_sp(s - groups)
    can_right, can_left = h + 1 < heads, h > 0
    onward = ((right, can_right), (left, can_left))
    weights = (wq, wk, wv)
    peers = [at_sp(h * groups + lax.rem(r + e, groups)) for e in range(1, groups)]
    others = [lax.rem(r + e, groups) for e in range(1, groups)]

    loads = {"tok": pltpu.make_async_copy(tok, x.at[ds(h, rows), :], local_sem.at[0])}
    for i in (V, K, Q):
        loads["own", i] = pltpu.make_async_copy(weights[i], wown.at[i], local_sem.at[1 + i])
        loads["mine", i] = pltpu.make_async_copy(
            weights[i].at[:, ds(h, vdim)], w_at(s, i), local_sem.at[4 + i]
        )
    loads["lam"] = pltpu.make_async_copy(lam_in, lam, local_sem.at[7])
    loads["gain"] = pltpu.make_async_copy(gain_in, gain, local_sem.at[8])
    for c in range(halves):
        loads["out", c] = pltpu.make_async_copy(
            wo_in.at[:, pl.ds(c * hcols, hcols)], wo.at[h * halves + c], local_sem.at[9 + c]
        )
    for copy in loads.values():
        copy.start()

    def loaded(key):
        if key in loads:
            loads.pop(key).wait()

    pl.semaphore_wait(barrier, heads + groups - 2 + len(bits))

    def send_tokens():
        loaded("tok")
        for c in range(chunks):
            for target, can in onward:
                send(x_at(h, t, c), x_at(h, t, c), TOKENS_Z, xz_recv.at[h, c], target, can)

    def send_own_weight(i):
        loaded(("mine", i))
        for peer in peers:
            send(w_at(s, i), w_at(s, i), WEIGHTS_Y, wy_recv.at[i], peer)

    def send_weight(i, d):
        loaded(("own", i))
        for owner, cond in ((h + d, h + d < heads), (h - d, h - d >= 0)):
            safe = jnp.where(cond, owner, h)
            send(wown.at[i, :, ds(safe, vdim)], w_at(s, i), WEIGHTS_Z, wz_recv.at[h, i],
                 at_sp(safe * groups + r), cond)

    spread = [(v, [b for b in reversed(bits) if v == 0 or b < (v & -v)]) for v in range(parts)]
    relays = [v for v, along in spread if v and along]
    leaves = parts - 1 - len(relays)

    def part_of(v):
        part = t
        for b in bits:
            if v & b:
                part = flip(part, b)
        return part

    def spread_sem(block, v, c):
        return xx_recv.at[block, relays.index(v), c] if v in relays else xe_recv.at[block]

    def pass_on(block, v, c, cond):
        piece = x_at(block, part_of(v), c)
        for b in spread[v][1]:
            send(piece, piece, SPREAD, spread_sem(block, v | b, c), at_tp(flip(t, b)), cond)

    def reach(k):
        if k == 0:
            return [(h, None, 0)]
        return [
            (jnp.where(have, block, h), have, side)
            for side, (block, have) in enumerate(((h - k, h - k >= 0), (h + k, h + k < heads)))
        ]

    def when(have, body):
        if have is None:
            body()
        else:
            pl.when(have)(body)

    def relay_tokens(k, c):
        for safe, have, side in reach(k):
            when(have, lambda safe=safe: arrived(x_at(safe, t, c), xz_recv.at[safe, c]))
            if k < heads - 1:
                target, can = onward[side]
                send(x_at(safe, t, c), x_at(safe, t, c), TOKENS_Z, xz_recv.at[safe, c], target,
                     jnp.logical_and(have, can))
            pass_on(safe, 0, c, have)

    def spread_tokens(k, c):
        for v in sorted(relays, reverse=True):
            for safe, have, _ in reach(k):
                when(have, lambda safe=safe: arrived(x_at(safe, part_of(v), c), spread_sem(safe, v, c)))
                pass_on(safe, v, c, have)

    def have_tokens(k):
        for safe, have, _ in reach(k):
            when(have, lambda safe=safe: arrived(x.at[ds(safe, rows), :leaves * seg], xe_recv.at[safe]))

    def forward_weight(i, d):
        for source_h, have, _ in reach(d):
            piece = w_at(source_h * groups + r, i)
            when(have, lambda piece=piece, source_h=source_h: arrived(piece, wz_recv.at[source_h, i]))
            for peer in peers:
                send(piece, piece, WEIGHTS_Y, wy_recv.at[i], peer, have)

    def have_weight(i):
        arrived(w.at[:(groups - 1) * heads * depth, pl.ds(i * vdim, vdim)], wy_recv.at[i])

    def begin_queries():
        loaded("tok")
        loaded(("mine", Q))
        if by_source:
            acc[...] = query_product(r)

    def query_product(group):
        total = None
        for k in range(heads):
            source = k * groups + group
            term = jnp.dot(x[:, ds(source, depth)], w[ds(source, depth), :vdim],
                           preferred_element_type=jnp.float32)
            total = term if total is None else total + term
        return total

    def finish_queries():
        if not by_source:
            full = jnp.dot(x[...], w[:, :vdim], preferred_element_type=jnp.float32)
        else:
            full = acc[...]
            for other in others:
                full = full + query_product(other)
        qb[...] = full.astype(jnp.bfloat16)

    def share_rows(k):
        loaded("tok")
        loaded(("mine", K))
        loaded(("mine", V))

        def body(block):
            mine = ds(block * groups + r, rows)
            kv[mine, :] = jnp.dot(
                x[ds(block, rows), :], w[:, vdim:], preferred_element_type=jnp.float32
            ).astype(jnp.bfloat16)
            for peer in peers:
                send(kv.at[mine, :], kv.at[mine, :], KEYS_Y, kv_recv.at[block], peer)

        for safe, have, _ in reach(k):
            when(have, lambda safe=safe: body(safe))

    def send_out_weight(c):
        if c >= halves:
            return
        loaded(("out", c))
        piece = h * halves + c
        for target, can in onward:
            send(wo.at[piece], wo.at[piece], OUT_Z, wo_recv.at[piece], target, can)

    def relay_out_weight(k, c):
        if c >= halves:
            return
        for safe, have, side in reach(k):
            piece = safe * halves + c
            when(have, lambda piece=piece: arrived(wo.at[piece], wo_recv.at[piece]))
            if k < heads - 1:
                target, can = onward[side]
                send(wo.at[piece], wo.at[piece], OUT_Z, wo_recv.at[piece], target,
                     jnp.logical_and(have, can))

    lane = lax.broadcasted_iota(jnp.int32, (rows, vdim), 1)
    factor = (vdim // 2) ** (-0.5) * 1.4426950408889634
    seen = []

    def attend(k):
        for j in range(k + 1):
            if j not in seen:
                seen.append(j)
                arrived(kv.at[:(groups - 1) * rows, :], kv_recv.at[j])
        loaded("lam")
        loaded("gain")
        lam_here = jnp.float32(0.0)
        for j in range(heads):
            lam_here = jnp.where(h == j, lam[j], lam_here)
        extent = (k + 1) * groups * rows
        q_rows = qb[k * rows:(k + 1) * rows, :]
        keys = kv[:extent, :vdim]
        values = kv[:extent, vdim:]
        clear = k * groups * rows // 128 * 128
        edge = extent - clear
        row = lax.broadcasted_iota(jnp.int32, (2 * rows, edge), 0)
        row = jnp.where(row >= rows, row - rows, row)
        ahead = lax.broadcasted_iota(jnp.int32, (2 * rows, edge), 1) + clear - row
        visible = ahead <= (k * groups + r) * rows
        zero = jnp.zeros_like(q_rows)
        both = jnp.concatenate(
            [jnp.where(lane < vdim // 2, q_rows, zero), jnp.where(lane >= vdim // 2, q_rows, zero)]
        )
        scores = lax.dot_general(
            both, keys, (((1,), (1,)), ((), ())), preferred_element_type=jnp.float32
        )
        parts_of = [jnp.where(visible, scores[:, clear:], -1e30)]
        if clear:
            parts_of.insert(0, scores[:, :clear])
        top = functools.reduce(
            jnp.maximum, [jnp.max(part, axis=-1, keepdims=True) for part in parts_of]
        )
        total, mixed, start = None, None, 0
        for part in parts_of:
            e = jnp.exp2((part - top) * factor)
            size = part.shape[-1]
            term = jnp.sum(e, axis=-1, keepdims=True)
            product = jnp.dot(
                e.astype(jnp.bfloat16), values[start:start + size], preferred_element_type=jnp.float32
            )
            total = term if total is None else total + term
            mixed = product if mixed is None else mixed + product
            start += size
        mixed = mixed / total
        maps = (mixed[:rows], mixed[rows:])
        mixture = maps[0] - lam_here * maps[1]
        normalized = (
            mixture
            * lax.rsqrt(jnp.mean(mixture * mixture, axis=-1, keepdims=True) + 1e-05)
            * gain[...]
        )
        ho_out[k] = normalized.astype(jnp.bfloat16)
        send(ho_out.at[k], ho.at[r, h], HEADS_Z, ho_recv.at[h], at_sp(k * groups + r), k != h)

        @pl.when(k == h)
        def _():
            ho[r, h] = ho_out[k]

    def forward_heads(d):
        for source, have, _ in reach(d):
            if d:
                when(have, lambda source=source: arrived(ho.at[r, source], ho_recv.at[source]))
            for peer in peers:
                send(ho.at[r, source], ho.at[r, source], HEADS_Y, hof_recv.at[0], peer, have)

    def have_heads():
        arrived(ho.at[:groups - 1], hof_recv.at[0])

    buddy = at_tp(flip(t, 1))
    members = [r] + others

    def column_block(pair, which):
        return 2 * lax.rem(lax.div(h, 2) + pair, pairs) + lax.rem(h + which, 2)

    def pieces_of(later, p):
        pair, half = p // 2, p % 2
        if half >= halves:
            return []
        return [
            (e, pair, half, (e * pairs + pair) * halves + half)
            for e in (range(1, groups) if later else range(1))
        ]

    def partial_product(e, pair, half, which):
        lhs = jnp.concatenate([ho[members[e], k] for k in range(heads)], axis=-1)
        return jnp.dot(lhs, wo[column_block(pair, which) * halves + half],
                       preferred_element_type=jnp.float32)

    def project_theirs(later, p):
        for e, pair, half, j in pieces_of(later, p):
            part_out[j] = partial_product(e, pair, half, 1 - low).astype(jnp.bfloat16)
            send(part_out.at[j], part_in.at[j], PARTS, p_recv.at[j], buddy)

    def project_mine(later, p):
        for e, pair, half, j in pieces_of(later, p):
            own = partial_product(e, pair, half, low)
            arrived(part_in.at[j], p_recv.at[j])
            sum_out[0, j] = (own + part_in[j].astype(jnp.float32)).astype(jnp.bfloat16)
            send(sum_out.at[0, j], sum_in.at[0, j], SUMS, s_recv.at[0, j], at_tp(flip(t, bits[1])))

    def add_up(later, p):
        last = len(bits) - 1
        for e, pair, half, j in pieces_of(later, p):
            for i in range(1, len(bits)):
                arrived(sum_in.at[i - 1, j], s_recv.at[i - 1, j])
                total = (
                    sum_out[i - 1, j].astype(jnp.float32) + sum_in[i - 1, j].astype(jnp.float32)
                ).astype(jnp.bfloat16)
                if i < last:
                    sum_out[i, j] = total
                    send(sum_out.at[i, j], sum_in.at[i, j], SUMS, s_recv.at[i, j],
                         at_tp(flip(t, bits[i + 1])))
            place = (column_block(pair, low) * groups + r) * halves + half
            if e == 0:
                staged[place] = total
                send(staged.at[place], staged.at[place], RESULTS, d_recv.at[0], buddy)
            else:
                sum_out[last, j] = total
                send(sum_out.at[last, j], staged.at[place], RESULTS_Y, f_recv.at[r, p], peers[e - 1])

    def finished(p):
        for e, pair, half, _ in pieces_of(True, p):
            place = (column_block(pair, low) * groups + members[e]) * halves + half
            arrived(staged.at[place], f_recv.at[members[e], p])
            send(staged.at[place], staged.at[place], RESULTS, d_recv.at[0], buddy)

    def all_finished():
        arrived(part_in, d_recv.at[0])

    index = {"q": Q, "k": K, "v": V}
    run = {
        "t": lambda k, c=0: relay_tokens(int(k), int(c)) if int(k) else send_tokens(),
        "m": lambda k, c: spread_tokens(int(k), int(c)),
        "e": lambda k: have_tokens(int(k)),
        "y": lambda i: send_own_weight(index[i]),
        "W": lambda i, d: send_weight(index[i], int(d)),
        "f": lambda i, d: forward_weight(index[i], int(d)),
        "h": lambda i: have_weight(index[i]),
        "b": lambda k: share_rows(int(k)),
        "g": lambda i: begin_queries(),
        "d": lambda i: finish_queries(),
        "O": lambda c: send_out_weight(int(c)),
        "o": lambda k, c: relay_out_weight(int(k), int(c)),
        "a": lambda k: attend(int(k)),
        "r": lambda d: forward_heads(int(d)),
        "P": lambda e, p: project_theirs(int(e), int(p)),
        "S": lambda e, p: project_mine(int(e), int(p)),
        "H": have_heads,
        "X": lambda e, p: add_up(int(e), int(p)),
        "F": lambda p: finished(int(p)),
        "Z": all_finished,
    }
    for name in PLAN:
        run[name[0]](*name[1:])

    for place in range(n * halves):
        out[:, place * hcols:(place + 1) * hcols] = staged[place]
    inner = jnp.logical_and(can_right, can_left)
    blocks = heads + 1
    out_rows = blocks * heads * vdim * ocols // width
    pl.when(inner)(lambda: arrived(x.at[:, :blocks * seg // heads], sent.at[TOKENS_Z]))
    pl.when(jnp.logical_not(inner))(lambda: arrived(x.at[:rows, :seg], sent.at[TOKENS_Z]))
    pl.when(inner)(lambda: arrived(x.at[:out_rows, :], sent.at[OUT_Z]))
    pl.when(jnp.logical_not(inner))(lambda: arrived(wo.at[:halves], sent.at[OUT_Z]))
    arrived(wown.at[:, :, :(heads - 1) * vdim], sent.at[WEIGHTS_Z])
    arrived(w.at[:(groups - 1) * heads * depth, :], sent.at[WEIGHTS_Y])
    arrived(x.at[:, :(heads - 1) * (parts - 1) * seg // heads], sent.at[SPREAD])
    arrived(kv.at[:heads * (groups - 1) * rows, :], sent.at[KEYS_Y])
    arrived(ho_out.at[:heads - 1], sent.at[HEADS_Z])
    arrived(ho.at[:groups - 1], sent.at[HEADS_Y])
    arrived(part_out, sent.at[PARTS])
    arrived(sum_out.at[:len(bits) - 1], sent.at[SUMS])
    arrived(part_out.at[:(groups - 1) * pairs * halves], sent.at[RESULTS_Y])
    arrived(part_out, sent.at[RESULTS])


def solution(mesh):
    n, parts = mesh.shape["sp"], mesh.shape["tp"]

    def step(tokens, query_weight, key_weight, value_weight, out_weight, mix_lambda, head_gain):
        rows, width = tokens.shape
        heads = mix_lambda.shape[0]
        vdim = head_gain.shape[0]
        depth = query_weight.shape[0]
        groups = n // heads
        ocols = out_weight.shape[1]
        pairs = heads // 2
        halves = 2 if ocols % 256 == 0 else 1
        hcols = ocols // halves
        pieces = groups * pairs * halves
        nbits = parts.bit_length() - 1
        chunks = 2
        dma = pltpu.SemaphoreType.DMA
        bf16 = jnp.bfloat16
        limit = 32 * 1024 if n * rows <= 2048 else 60000
        operands = [pltpu.with_memory_space_constraint(operand, pltpu.HBM) for operand in (
            tokens, query_weight, key_weight, value_weight, out_weight, mix_lambda,
            head_gain.reshape(1, vdim),
        )]
        return pl.pallas_call(
            functools.partial(kernel, n, parts, heads, chunks),
            out_shape=pltpu.VMEM((rows, width), bf16),
            in_specs=[pl.BlockSpec(memory_space=pltpu.HBM)] * 7,
            out_specs=pl.BlockSpec(memory_space=pltpu.VMEM),
            scratch_shapes=[
                pltpu.VMEM((heads * rows, width), bf16),
                pltpu.VMEM((3, depth, heads * vdim), bf16),
                pltpu.VMEM((width, 3 * vdim), bf16),
                pltpu.VMEM((heads * rows, vdim), jnp.float32),
                pltpu.VMEM((heads * rows, vdim), bf16),
                pltpu.VMEM((n * rows, 2 * vdim), bf16),
                pltpu.VMEM((heads * halves, heads * vdim, hcols), bf16),
                pltpu.VMEM((heads, rows, vdim), bf16),
                pltpu.VMEM((groups, heads, rows, vdim), bf16),
                pltpu.VMEM((pieces, rows, hcols), bf16),
                pltpu.VMEM((pieces, rows, hcols), bf16),
                pltpu.VMEM((nbits, pieces, rows, hcols), bf16),
                pltpu.VMEM((nbits, pieces, rows, hcols), bf16),
                pltpu.VMEM((n * halves, rows, hcols), bf16),
                pltpu.VMEM((1, vdim), jnp.float32),
                pltpu.SMEM((heads,), jnp.float32),
                dma((11,)), dma((12,)),
                dma((heads, chunks)), dma((heads, parts // 2 - 1, chunks)), dma((heads,)),
                dma((heads, 3)), dma((3,)), dma((heads,)), dma((heads * halves,)), dma((heads,)),
                dma((1,)), dma((pieces,)), dma((nbits - 1, pieces)), dma((groups, pairs * 2)), dma((1,)),
            ],
            compiler_params=pltpu.CompilerParams(
                collective_id=0, has_side_effects=True, vmem_limit_bytes=limit * 1024
            ),
        )(*operands)

    placed = (
        P("sp", None),
        P("sp", "tp"),
        P("sp", "tp"),
        P("sp", "tp"),
        P("tp", "sp"),
        P("tp"),
        P(),
    )
    return jax.shard_map(step, mesh=mesh, in_specs=placed, out_specs=P("sp", None), check_vma=False)
```
